32 devices in a mesh: kv: 8 (over z, x), tp: 4 (over y, core).
Axes of the slice: x: 2, y: 2, z: 4, core: 2. Of those that a mesh axis runs over, the one named last changes fastest.
Arguments:
- tokens: bfloat16 [96, 4096], P(None, 'kv'), may hold values from -210 to 210
- norm_gain: float32 [4096], P('kv'), may hold values from 0.1 to 1.9
- w_query: bfloat16 [4096, 4096], P('kv', 'tp'), may hold values from -1 to 1
- w_key: bfloat16 [4096, 4096], P('kv', 'tp'), may hold values from -2 to 2
- w_value: bfloat16 [4096, 4096], P('kv', 'tp'), may hold values from -0.09375 to 0.09375
- w_output: bfloat16 [4096, 4096], P('tp', 'kv'), may hold values from -0.09375 to 0.09375
- cache_keys: bfloat16 [4, 4096, 4096], P(None, 'kv', 'tp'), may hold values from -820 to 820
- cache_values: bfloat16 [4, 4096, 4096], P(None, 'kv', 'tp'), may hold values from -6 to 6
- map_lambda: float32 [64], P('tp'), may hold values from 0.3 to 0.8
- out_gain: float32 [4096], P('tp'), may hold values from 0.1 to 1.9
- parents: int32 [4, 24], replicated, may hold values from -1 to 22, as said below
- lengths: int32 [4], replicated, may hold values from 2048 to 4048, as said below
- accepted: int32 [4], replicated, may hold values from 0 to 24
Outputs:
- mixed: bfloat16 [96, 4096], P(None, 'kv')
- new_keys: bfloat16 [4, 4096, 4096], P(None, 'kv', 'tp')
- new_values: bfloat16 [4, 4096, 4096], P(None, 'kv', 'tp')
The draws below stay inside these ranges and needn't reach their ends.
Inputs may be any that keep to these rules, and one draw needn't show every extreme that they name: parents[b, j] lies between -1 and j - 1. `lengths`: some sequence has exactly the largest value.
All inputs are finite; a program needn't handle non-finite values.
Results may differ from the reference program's by a relative error of at most 0.029.
Values may be sent and summed in bfloat16 or wider, within the bound.
A program may use at most 128 MiB of HBM per device.

```python
import math
import jax
import jax.numpy as jnp
from jax import lax

D = 4096
HEADS = 64
HEAD = 64
QK = 32
SEQS = 4
POS_DEV = 512
PROP = 24
CACHE = 4096
ROWS = 96
N_KV = 8
N_TP = 4


def draw_tokens(key, part):
    column_rise = jnp.arange(D, dtype=jnp.float32) / (D - 1)
    shared_part = 0.8 ** 0.5
    own_part = 0.2 ** 0.5
    common = jax.random.normal(jax.random.fold_in(key, 11), (SEQS, 1, D), jnp.float32)
    own = jax.random.normal(key, (SEQS, PROP, D), jnp.float32)
    mixture = jnp.clip(shared_part * common + own_part * own, -6.0, 6.0).reshape(ROWS, D)
    values = mixture * jnp.exp(column_rise * 1.1)
    return values.astype(jnp.bfloat16)


def query_matrix(key):
    base = jnp.clip(jax.random.normal(jax.random.fold_in(key, 21), (D, HEADS * HEAD), jnp.float32), -6.0, 6.0)
    return base * D ** (-0.5)


def draw_w_query(key, part):
    return query_matrix(key).astype(jnp.bfloat16)


def draw_w_key(key, part):
    coupling = math.log(1.6 * CACHE) / math.sqrt(QK)
    noise = jnp.clip(jax.random.normal(jax.random.fold_in(key, 22), (D, HEADS * HEAD), jnp.float32), -6.0, 6.0)
    values = coupling * query_matrix(key) + noise * D ** (-0.5)
    return values.astype(jnp.bfloat16)


def draw_cache_keys(key, part):
    values = 1.7 * jnp.clip(jax.random.normal(key, (SEQS, CACHE, HEADS * HEAD), jnp.float32), -6.0, 6.0)
    return values.astype(jnp.bfloat16)


def draw_parents(key, part):
    limits = jnp.arange(PROP, dtype=jnp.int32)
    return jax.random.randint(key, (SEQS, PROP), -1, limits[None, :]).astype(jnp.int32)


def draw_lengths(key, part):
    drawn = jax.random.randint(key, (SEQS,), CACHE // 2, CACHE - 2 * PROP + 1)
    chosen = jax.random.randint(jax.random.fold_in(key, 1), (), 0, SEQS)
    return drawn.at[chosen].set(CACHE - 2 * PROP).astype(jnp.int32)


def with_ends(array, stream_key, least, high):
    longest = array.shape.index(max(array.shape))
    spots = []
    for shift in (0, 1):
        where = [jax.random.randint(jax.random.fold_in(stream_key, axis), (), 0, length) for axis, length in enumerate(array.shape)]
        where[longest] = (where[longest] + shift) % array.shape[longest]
        spots.append(tuple(where))
    return array.at[spots[0]].set(least).at[spots[1]].set(high)


def block_levels(own_key, extent, shards, smallest, largest):
    factor_of = 1.0
    for position, shards_of in shards:
        heights = jax.random.uniform(jax.random.fold_in(jax.random.fold_in(own_key, 6), position), (shards_of,), jnp.float32, smallest / len(shards), largest / len(shards))
        factor_of = factor_of * jnp.repeat(jnp.exp(heights), extent[position] // shards_of).reshape((-1,) + (1,) * (len(extent) - 1 - position))
    return factor_of


def bell_draw(own_key, shape, scale, reach, split=(), kind=jnp.bfloat16):
    values = scale * jax.random.normal(own_key, shape, jnp.float32)
    if split:
        values = values * block_levels(own_key, shape, split, -0.22, 0.18)
    return jnp.clip(values, -reach, reach).astype(kind)


def setup_inputs(seed: int = 0) -> dict:
    keys = jax.random.split(jax.random.key(seed), 14)
    tokens = draw_tokens(jax.random.fold_in(keys[13], 71), 0)
    norm_gain = jnp.clip(1.0 + 0.18 * jax.random.normal(keys[1], (D,), jnp.float32), 0.1, 1.9)
    w_query = draw_w_query(jax.random.fold_in(keys[13], 71), 0)
    w_key = draw_w_key(jax.random.fold_in(keys[13], 71), 0)
    w_value = bell_draw(keys[4], (D, HEADS * HEAD), D ** -0.5, 0.09375, ((0, 8), (1, 4)))
    w_output = bell_draw(keys[5], (HEADS * HEAD, D), (HEADS * HEAD) ** -0.5, 0.09375, ((0, 4), (1, 8)))
    cache_keys = draw_cache_keys(jax.random.fold_in(keys[13], 71), 0)
    cache_values = bell_draw(keys[7], (SEQS, CACHE, HEADS * HEAD), 1.0, 6.0, ((1, 8), (2, 4)))
    map_lambda = jnp.clip(0.3 + 0.5 * jax.random.uniform(keys[8], (HEADS,), jnp.float32) ** block_levels(keys[8], (HEADS,), ((0, 4),), -0.2, 0.2), 0.3, 0.8)
    out_gain = jnp.clip(1.0 + 0.18 * jax.random.normal(keys[9], (HEADS * HEAD,), jnp.float32), 0.1, 1.9)
    parents = draw_parents(jax.random.fold_in(keys[13], 71), 0)
    lengths = draw_lengths(jax.random.fold_in(keys[13], 71), 0)
    accepted = with_ends(jax.random.randint(keys[12], (SEQS,), 0, PROP + 1), jax.random.fold_in(keys[12], 1), 0, PROP).astype(jnp.int32)
    return dict(tokens=tokens, norm_gain=norm_gain, w_query=w_query, w_key=w_key, w_value=w_value, w_output=w_output, cache_keys=cache_keys, cache_values=cache_values, map_lambda=map_lambda, out_gain=out_gain, parents=parents, lengths=lengths, accepted=accepted)


epsilon = 1e-05
masked_low = -1e+30

def ancestry(parents):
    count = parents.shape[1]
    places = jnp.arange(count, dtype=jnp.int32)
    parent_links = (parents[:, :, None] == places[None, None, :]).astype(jnp.float32)
    identity = jnp.eye(count, dtype=jnp.float32)[None]

    def extend(turn_index, reached):
        return jnp.minimum(1.0, identity + jnp.einsum('bji,bik->bjk', parent_links, reached))
    reached = lax.fori_loop(0, count, extend, jnp.broadcast_to(identity, parent_links.shape))
    return reached > 0.5

def reference(tokens, norm_gain, w_query, w_key, w_value, w_output, cache_keys, cache_values, map_lambda, out_gain, parents, lengths, accepted):
    f32 = jnp.float32
    bf16 = jnp.bfloat16
    tokens_wide = tokens.astype(f32)
    norm_factor = lax.rsqrt(lax.optimization_barrier(jnp.mean(tokens_wide * tokens_wide, axis=1, keepdims=True)) + epsilon)
    gained = (tokens_wide * norm_gain).astype(bf16)

    def projection(weight_matrix):
        return (jnp.dot(gained, weight_matrix, preferred_element_type=f32) * norm_factor).astype(bf16)
    queries = projection(w_query)
    keys_flat = projection(w_key)
    values_flat = projection(w_value)
    query_heads = queries.astype(f32).reshape(SEQS, PROP, HEADS, 2, QK)
    key_heads = keys_flat.astype(f32).reshape(SEQS, PROP, HEADS, 2, QK)
    value_heads = values_flat.reshape(SEQS, PROP, HEADS, HEAD)
    start = lengths + accepted
    score_scale = QK ** (-0.5)

    def cache_block(block_index):
        begin = (block_index * POS_DEV).astype(jnp.int32)
        block_keys = lax.dynamic_slice_in_dim(cache_keys, begin, POS_DEV, 1).astype(f32)
        block_keys = block_keys.reshape(SEQS, POS_DEV, HEADS, 2, QK)
        block_vals = lax.dynamic_slice_in_dim(cache_values, begin, POS_DEV, 1).astype(f32)
        block_vals = block_vals.reshape(SEQS, POS_DEV, HEADS, HEAD)
        positions = begin + jnp.arange(POS_DEV, dtype=jnp.int32)
        visible = (positions[None, :] < start[:, None])[:, None, None, None, :]
        scores = jnp.einsum('bqhmd,bkhmd->bmhqk', query_heads, block_keys) * score_scale
        block_max = lax.optimization_barrier(jnp.max(jnp.where(visible, scores, masked_low), axis=-1))
        block_weight = jnp.where(visible, jnp.exp(scores - block_max[..., None]), 0.0)
        block_total = lax.optimization_barrier(jnp.sum(block_weight, axis=-1))
        rounded = block_weight.astype(bf16).astype(f32)
        block_values = jnp.einsum('bmhqk,bkhd->bmhqd', rounded, block_vals).astype(bf16)
        return (block_max, block_total, block_values)
    maxima, totals, values = lax.map(cache_block, jnp.arange(N_KV, dtype=jnp.int32))
    cache_max = lax.optimization_barrier(jnp.max(maxima, axis=0))
    factors = jnp.exp(maxima - cache_max[None])
    cache_total = lax.optimization_barrier(jnp.sum(totals * factors, axis=0))
    cache_sum = lax.optimization_barrier(jnp.sum(values.astype(f32) * factors[..., None], axis=0))
    lineage = ancestry(parents)[:, None, None, :, :]
    self_scores = jnp.einsum('bqhmd,bjhmd->bmhqj', query_heads, key_heads) * score_scale
    self_max = lax.optimization_barrier(jnp.max(jnp.where(lineage, self_scores, masked_low), axis=-1))
    top = jnp.maximum(cache_max, self_max)
    self_weight = jnp.where(lineage, jnp.exp(self_scores - top[..., None]), 0.0)
    carried = jnp.exp(cache_max - top)
    denominator = cache_total * carried + lax.optimization_barrier(jnp.sum(self_weight, axis=-1))
    self_values = jnp.einsum('bmhqj,bjhd->bmhqd', self_weight.astype(bf16).astype(f32), value_heads.astype(f32))
    attended = (cache_sum * carried[..., None] + self_values) / denominator[..., None]
    difference = attended[:, 0] - map_lambda[None, :, None, None] * attended[:, 1]
    gains = out_gain.reshape(HEADS, HEAD)[None, :, None, :]
    normed = difference * lax.rsqrt(lax.optimization_barrier(jnp.mean(difference * difference, axis=-1, keepdims=True)) + epsilon) * gains
    normed = jnp.transpose(normed, (0, 2, 1, 3)).reshape(ROWS, HEADS * HEAD).astype(bf16)
    group = HEADS // N_TP
    pieces = normed.reshape(ROWS, N_TP, group * HEAD).astype(f32)
    weight_groups = w_output.reshape(N_TP, group * HEAD, D).astype(f32)
    partials = jnp.einsum('rgc,gcd->grd', pieces, weight_groups).astype(bf16)
    partials = lax.optimization_barrier(partials).astype(f32)
    mixed = lax.optimization_barrier(jnp.sum(partials, axis=0)).astype(bf16)

    def place(cache_row, new_rows, begin):
        return lax.dynamic_update_slice(cache_row, new_rows, (begin, jnp.int32(0)))
    new_keys = jax.vmap(place)(cache_keys, keys_flat.reshape(SEQS, PROP, HEADS * HEAD), start)
    new_values = jax.vmap(place)(cache_values, values_flat.reshape(SEQS, PROP, HEADS * HEAD), start)
    return (mixed, new_keys, new_values)
```

```python
import functools
import math

import jax
import jax.numpy as jnp
from jax import lax
from jax.experimental import pallas as pl
from jax.experimental.pallas import tpu as pltpu
from jax.sharding import PartitionSpec as P

HEAD = 64
QK = 32
LANES = 128
epsilon = 1e-05
masked_low = -1e30
MESH = pl.DeviceIdType.MESH
f32 = jnp.float32
bf16 = jnp.bfloat16


def iota(shape, dim):
    return lax.broadcasted_iota(jnp.int32, shape, dim)


def greet(axes):
    barrier = pltpu.get_barrier_semaphore()
    count = 0
    for axis, n in axes:
        me = lax.axis_index(axis)
        for k in range(1, n):
            pl.semaphore_signal(
                barrier, inc=1, device_id={axis: lax.rem(me + k, n)}, device_id_type=MESH
            )
            count += 1
    return barrier, count


def remote(src, dst, send_sem, recv_sem, axis, to):
    return pltpu.make_async_remote_copy(
        src_ref=src,
        dst_ref=dst,
        send_sem=send_sem,
        recv_sem=recv_sem,
        device_id={axis: to},
        device_id_type=MESH,
    )


def drain(ref, sem):
    pltpu.make_async_copy(ref, ref, sem).wait()


def flip(i, bit):
    return i + bit - 2 * bit * lax.rem(i // bit, 2)


def main_kernel(
    n, t, cols, seqs, prop, features, inner_n,
    tok_hbm, gain_hbm, lam_hbm, out_gain_hbm, parent_hbm, len_hbm, acc_hbm,
    wq_hbm, wk_hbm, wv_hbm, wo_hbm, keys_hbm, vals_hbm,
    out_ref, kv_ref, kbuf, vbuf, len_out, acc_out,
    tok_ref, gain_ref, lam_ref, out_gain_ref, parent_ref, len_ref, acc_ref,
    wbuf, wo_buf, q_part, q_recv, q_all, kv_part, kvx_recv, kv_sum, kvz_recv, sq_all,
    bv, bv_recv, st, st_recv, self_v, self_st, norm_all, out_part, out_recv,
    s_in, w_in, k_in, v_in, sq_s, sq_r, q_s, q_r, qa_s, qa_r, kx_s, kx_r, kz_s, kz_r, up_s, up_r, ag_s, ag_r,
    b_s, b_r, st_s, st_r, g_s, g_r, t_s, t_r,
):
    me = lax.axis_index("kv")
    mine = lax.axis_index("tp")
    groups = n // cols
    rows = tok_ref.shape[0]
    part = rows // groups
    per = seqs // groups
    both = 2 * prop
    _, length, width = kbuf.shape
    scale = QK ** (-0.5)
    peers = [lax.rem(me + k, n) for k in range(1, n)]
    outer_n = n // inner_n
    half = outer_n // 2
    x, z = lax.rem(me, inner_n), me // inner_n
    x_peers = [lax.rem(x + k, inner_n) for k in range(1, inner_n)]
    slot = lax.rem(z, half) * inner_n + x
    flat = half * inner_n - 1
    barrier, count = greet((("kv", n), ("tp", t)))
    weights = [
        pltpu.make_async_copy(src, dst, w_in.at[i])
        for i, (src, dst) in enumerate(
            ((wq_hbm, wbuf.at[0]), (wk_hbm, wbuf.at[1]), (wv_hbm, wbuf.at[2]), (wo_hbm, wo_buf))
        )
    ]
    small = [
        pltpu.make_async_copy(src, dst, s_in.at[i])
        for i, (src, dst) in enumerate(
            (
                (tok_hbm, tok_ref), (gain_hbm, gain_ref), (lam_hbm, lam_ref), (out_gain_hbm, out_gain_ref),
                (parent_hbm, parent_ref), (len_hbm, len_ref), (acc_hbm, acc_ref), (len_hbm, len_out), (acc_hbm, acc_out),
            )
        )
    ]
    order = [r * per + p for p in range(per) for r in range(groups)]
    loads = {}
    for b in order:
        loads[b] = (
            pltpu.make_async_copy(keys_hbm.at[b], kbuf.at[b], k_in.at[b]),
            pltpu.make_async_copy(vals_hbm.at[b], vbuf.at[b], v_in.at[b]),
        )
    for copy in small[:2] + weights[:1] + small[2:] + weights[1:3]:
        copy.start()
    for b in order:
        for copy in loads[b]:
            copy.start()
    weights[3].start()
    for copy in small[:2]:
        copy.wait()

    wide = tok_ref[...].astype(f32)
    square = jnp.sum(wide * wide, axis=1, keepdims=True)
    diagonal = iota((rows, LANES), 0) == iota((rows, LANES), 1)
    as_row = jnp.sum(jnp.where(diagonal, square, 0.0), axis=0, keepdims=True)
    sq_all[me] = as_row
    gained = (wide * gain_ref[...]).astype(bf16)

    def products(which, place):
        weights[which].wait()
        product = jnp.dot(gained, wbuf[which], preferred_element_type=f32)
        for c in range(cols):
            for b in range(seqs):
                place(
                    b % per,
                    c * groups + b // per,
                    product[b * prop : (b + 1) * prop, c * LANES : (c + 1) * LANES].astype(bf16),
                )

    def place_q(p, d, piece):
        q_part[p, d] = piece

    def place_k(p, d, piece):
        kv_part[d % inner_n, d // inner_n, p * prop : (p + 1) * prop, :LANES] = piece

    def place_v(p, d, piece):
        kv_part[d % inner_n, d // inner_n, p * prop : (p + 1) * prop, LANES:] = piece

    products(0, place_q)
    pl.semaphore_wait(barrier, count)
    for to in peers:
        remote(sq_all.at[me], sq_all.at[me], sq_s, sq_r, "kv", to).start()
    for p in range(per):
        for k, to in enumerate(peers):
            remote(q_part.at[p, to], q_recv.at[p, k], q_s, q_r.at[p], "kv", to).start()
    products(1, place_k)
    products(2, place_v)
    for k, to in enumerate(x_peers):
        remote(kv_part.at[to], kvx_recv.at[k], kx_s, kx_r, "kv", z * inner_n + to).start()

    lane = iota((1, LANES), 1)
    low = lane < HEAD
    for copy in small[2:]:
        copy.wait()
    own_first = lax.rem(me, groups) * per
    small_eye = iota((prop, prop), 0) == iota((prop, prop), 1)
    parent_rows = []
    for b in range(per):
        line = parent_ref[pl.ds(own_first + b, 1), :]
        parent_rows.append(
            jnp.sum(jnp.where(small_eye, line, 0), axis=1, keepdims=True)
        )
    parent = jnp.concatenate(parent_rows, axis=0)
    shape = (part, part)
    target = jnp.concatenate([p + b * prop for b, p in enumerate(parent_rows)], axis=0)
    link = (parent >= 0) & (target == iota(shape, 1))
    reach = jnp.where(link | (iota(shape, 0) == iota(shape, 1)), 1.0, 0.0)
    power = 1
    while power < prop:
        reach = jnp.minimum(
            jnp.dot(reach.astype(bf16), reach.astype(bf16), preferred_element_type=f32), 1.0
        )
        power *= 2
    lineage = jnp.concatenate([reach] * 4, axis=0) > 0.5

    drain(sq_all.at[pl.ds(0, n - 1)], sq_r)
    squares = sq_all[0]
    for k in range(1, n):
        squares = squares + sq_all[k]
    first = lax.rem(me, groups) * part
    picked = iota((part, LANES), 0) + first == iota((part, LANES), 1)
    mean = jnp.sum(jnp.where(picked, squares, 0.0), axis=1, keepdims=True) / features
    factor = lax.rsqrt(mean + epsilon)
    for p in range(per):
        drain(q_recv.at[p], q_r.at[p])
        total = q_part[p, me].astype(f32)
        for k in range(n - 1):
            total = total + q_recv[p, k].astype(f32)
        q_all[p, me] = (total * factor[p * prop : (p + 1) * prop]).astype(bf16)
        for to in peers:
            remote(q_all.at[p, me], q_all.at[p, me], qa_s, qa_r.at[p], "kv", to).start()

    def kv_across_x():
        drain(kvx_recv, kx_r)
        for i in range(outer_n):
            summed = kv_part[x, i].astype(f32)
            for k in range(inner_n - 1):
                summed = summed + kvx_recv[k, i].astype(f32)
            kv_sum[i] = summed.astype(bf16)

    chunks = [z]
    bits = []
    bit = 1
    while bit < outer_n:
        bits.append(bit)
        bit *= 2
    live = {}
    for s in reversed(range(len(bits))):
        live[s] = list(chunks)
        chunks = chunks + [flip(c, bits[s]) for c in chunks]

    def kv_send(s):
        partner = flip(z, bits[s])
        for i, c in enumerate(live[s]):
            remote(
                kv_sum.at[flip(c, bits[s])], kvz_recv.at[s, i], kz_s.at[s], kz_r.at[s], "kv", partner * inner_n + x
            ).start()

    def kv_take(s):
        size = len(live[s])
        drain(kvz_recv.at[s, pl.ds(0, size)], kz_r.at[s])
        drain(kvz_recv.at[s, pl.ds(0, size)], kz_s.at[s])
        for i, c in enumerate(live[s]):
            kv_sum[c] = (kv_sum[c].astype(f32) + kvz_recv[s, i].astype(f32)).astype(bf16)

    wide_lane = iota((1, 2 * LANES), 1)

    def attend(p):
        stat = jnp.zeros((both, LANES), f32)
        for r in range(groups):
            b = r * per + p
            rel = len_ref[b] + acc_ref[b] - me * length
            visible = iota((1, length), 1) < rel
            for copy in loads[b]:
                copy.wait()
            for g in range(width // (2 * LANES)):
                span = slice(g * 2 * LANES, (g + 1) * 2 * LANES)
                query = jnp.concatenate(
                    [q_all[p, c * groups + r].astype(f32) for c in (2 * g, 2 * g + 1)], axis=1
                )
                spread = jnp.concatenate(
                    [jnp.where(wide_lane // QK == i, query, 0.0) for i in range(2 * LANES // QK)],
                    axis=0,
                ).astype(bf16)
                scores = lax.dot_general(
                    spread, kbuf[b, :, span], (((1,), (1,)), ((), ())), preferred_element_type=f32
                )
                scores = jnp.where(visible, scores * scale, masked_low)
                largest = jnp.max(scores, axis=1, keepdims=True)
                weight = jnp.where(visible, jnp.exp(scores - largest), 0.0)
                total = jnp.sum(weight, axis=1, keepdims=True)
                summed = jnp.dot(weight.astype(bf16), vbuf[b, :, span], preferred_element_type=f32)
                merged = jnp.zeros((both, 2 * LANES), f32)
                for h in range(2 * LANES // HEAD):
                    piece = slice(h * both, (h + 1) * both)
                    merged = jnp.where(wide_lane // HEAD == h, summed[piece], merged)
                    at = ((2 * g + h // 2) * groups + r) * 4 + h % 2
                    stat = jnp.where(lane == at, largest[piece], stat)
                    stat = jnp.where(lane == at + 2, total[piece], stat)
                merged = merged.astype(bf16)
                for c in range(2):
                    bv[p, (2 * g + c) * groups + r] = merged[:, c * LANES : (c + 1) * LANES]
        turned = jnp.transpose(
            jnp.concatenate([stat, jnp.zeros((LANES - both, LANES), f32)], axis=0)
        )
        for d in range(n):
            st[p, d] = turned[4 * d : 4 * d + 4]
        for k, to in enumerate(peers):
            remote(st.at[p, to], st_recv.at[p, k], st_s, st_r.at[p], "kv", to).start()
        for k, to in enumerate(peers):
            remote(bv.at[p, to], bv_recv.at[p, k], b_s, b_r.at[p], "kv", to).start()

    def tree():
        own = (kv_sum[z].astype(f32) * factor).astype(bf16)
        kv_ref[slot, z // half] = own
        query = jnp.concatenate([q_all[p, me] for p in range(per)], axis=0).astype(f32)
        spread = jnp.concatenate(
            [jnp.where(lane // QK == i, query, 0.0) for i in range(4)], axis=0
        ).astype(bf16)
        scores = lax.dot_general(
            spread, own[:, :LANES], (((1,), (1,)), ((), ())), preferred_element_type=f32
        )
        scores = jnp.where(lineage, scores * scale, masked_low)
        top = jnp.max(scores, axis=1, keepdims=True)
        weight = jnp.where(lineage, jnp.exp(scores - top), 0.0)
        total = jnp.sum(weight, axis=1, keepdims=True)
        summed = jnp.dot(weight.astype(bf16), own[:, LANES:], preferred_element_type=f32)
        stat = jnp.zeros((both, LANES), f32)
        for p in range(per):
            cut = [slice(i * part + p * prop, i * part + (p + 1) * prop) for i in range(4)]

            def laid(array, head):
                return jnp.concatenate([array[cut[2 * head]], array[cut[2 * head + 1]]], axis=0)

            self_v[p] = jnp.where(low, laid(summed, 0), laid(summed, 1))
            for h in range(2):
                stat = jnp.where(lane == 4 * p + h, laid(top, h), stat)
                stat = jnp.where(lane == 4 * p + 2 + h, laid(total, h), stat)
        turned = jnp.transpose(
            jnp.concatenate([stat, jnp.zeros((LANES - both, LANES), f32)], axis=0)
        )
        for p in range(per):
            self_st[p] = turned[4 * p : 4 * p + 4]

    def kv_up():
        @pl.when(z < half)
        def _():
            remote(kv_ref.at[slot, 0], kv_ref.at[slot, 0], up_s, up_r, "kv", me + half * inner_n).start()

    def kv_spread():

        @pl.when(z >= half)
        def _():
            drain(kv_ref.at[slot, 0], up_r)
            for k in range(1, flat + 1):
                to = half * inner_n + lax.rem(slot + k, flat + 1)
                remote(kv_ref.at[slot], kv_ref.at[slot], ag_s, ag_r, "kv", to).start()

    def kv_end():

        @pl.when(z < half)
        def _():
            drain(kv_ref.at[slot, 0], up_s)

        @pl.when(z >= half)
        def _():
            for sem in (ag_r, ag_s):
                drain(kv_ref.at[pl.ds(0, flat)], sem)

    col = me // groups
    heads = iota(lam_ref.shape, 1)
    lam_low = jnp.sum(jnp.where(heads == 2 * col, lam_ref[...], 0.0), axis=1, keepdims=True)
    lam_high = jnp.sum(jnp.where(heads == 2 * col + 1, lam_ref[...], 0.0), axis=1, keepdims=True)
    lam = jnp.where(low, lam_low, lam_high)
    gain = out_gain_ref[:, pl.ds(pl.multiple_of(col * LANES, LANES), LANES)]

    def merge(p):
        drain(st_recv.at[p], st_r.at[p])
        drain(bv_recv.at[p], b_r.at[p])
        stats = [st[p, me]] + [st_recv[p, k] for k in range(n - 1)] + [self_st[p]]
        highest = functools.reduce(jnp.maximum, [a[:2] for a in stats])
        shares = [jnp.exp(a[:2] - highest) for a in stats]
        denominator = functools.reduce(lambda a, b: a + b, [a * b[2:] for a, b in zip(shares, stats)])
        inverse = 1.0 / denominator
        shares = [a * inverse for a in shares]
        filler = jnp.zeros((LANES - 2 * len(shares), LANES), f32)
        turned = jnp.transpose(jnp.concatenate(shares + [filler], axis=0))
        values = [bv[p, me]] + [bv_recv[p, k] for k in range(n - 1)] + [self_v[p]]
        attended = jnp.zeros((both, LANES), f32)
        for i, value in enumerate(values):
            share = jnp.where(low, turned[:both, 2 * i : 2 * i + 1], turned[:both, 2 * i + 1 : 2 * i + 2])
            attended = attended + value.astype(f32) * share
        difference = attended[:prop] - lam * attended[prop:]
        squared = difference * difference
        one = jnp.sum(jnp.where(low, squared, 0.0), axis=1, keepdims=True)
        two = jnp.sum(jnp.where(low, 0.0, squared), axis=1, keepdims=True)
        mean = jnp.where(low, one, two) / HEAD
        norm_all[p, me] = (difference * lax.rsqrt(mean + epsilon) * gain).astype(bf16)
        for to in peers:
            remote(norm_all.at[p, me], norm_all.at[p, me], g_s, g_r.at[p], "kv", to).start()

    def project(p):
        drain(q_recv.at[p], g_r.at[p])
        normed = jnp.concatenate(
            [
                jnp.concatenate([norm_all[p, c * groups + r] for r in range(groups)], axis=0)
                for c in range(cols)
            ],
            axis=1,
        )
        out_part[p] = jnp.dot(normed, wo_buf[...], preferred_element_type=f32).astype(bf16)
        for k in range(1, t):
            remote(out_part.at[p], out_recv.at[p, k - 1], t_s, t_r.at[p], "tp", lax.rem(mine + k, t)).start()

    def finish(p):
        drain(out_recv.at[p], t_r.at[p])
        mixed = out_part[p].astype(f32)
        for k in range(t - 1):
            mixed = mixed + out_recv[p, k].astype(f32)
        for r in range(groups):
            b = r * per + p
            out_ref[b * prop : (b + 1) * prop, :] = mixed[r * prop : (r + 1) * prop].astype(bf16)

    steps = [lambda: (kv_across_x(), kv_send(0))]
    for i in range(len(bits) - 1):
        steps.append(lambda i=i: (kv_take(i), kv_send(i + 1)))
    steps.append(lambda: (kv_take(len(bits) - 1), tree(), kv_up()))
    for p in range(per):
        drain(q_recv.at[p], qa_r.at[p])
        attend(p)
        if p in (0, 2):
            steps.pop(0)()
    while steps:
        steps.pop(0)()
    merged_upto = 0
    weights[3].wait()
    for p in range(merged_upto, per):
        merge(p)
        if p == 1 or p == per - 1 and per < 2:
            kv_spread()
    for p in range(per):
        project(p)
    for p in range(per):
        finish(p)
    kv_end()
    drain(sq_all.at[pl.ds(0, n - 1)], sq_s)
    drain(q_recv, q_s)
    drain(q_recv, qa_s)
    drain(kvx_recv, kx_s)
    drain(st_recv, st_s)
    drain(bv_recv, b_s)
    drain(q_recv, g_s)
    drain(out_recv, t_s)


def place_kernel(
    groups, prop, len_ref, acc_ref, mixed_ref, kv_ref, kbuf_in, vbuf_in, out_hbm, nk_hbm, nv_hbm, kbuf, vbuf,
    k_out, v_out, m_out,
):
    seqs, length, width = kbuf.shape
    cols = width // LANES
    per = seqs // groups
    chunks = kv_ref.shape[0]
    offset = lax.axis_index("kv") * length
    mixed = pltpu.make_async_copy(mixed_ref, out_hbm, m_out)
    mixed.start()
    stores = []
    window = 48
    for b in range(seqs):
        r, begin = b // per, (b % per) * prop
        rel = len_ref[b] + acc_ref[b] - offset
        base = jnp.clip((rel // 16) * 16, 0, length - window)
        at = pl.ds(pl.multiple_of(base, 16), window)
        slot = iota((window, prop), 0) + base - rel
        placing = (slot == iota((window, prop), 1)).astype(bf16)
        slot_col = iota((window, 1), 0) + base - rel
        inside = (slot_col >= 0) & (slot_col < prop)
        for which, buf in enumerate((kbuf, vbuf)):
            fresh = jnp.concatenate(
                [
                    kv_ref[
                        (c * groups + r) % chunks,
                        (c * groups + r) // chunks,
                        begin : begin + prop,
                        which * LANES : (which + 1) * LANES,
                    ]
                    for c in range(cols)
                ],
                axis=1,
            )
            moved = jnp.dot(placing, fresh, preferred_element_type=f32)
            old = buf[b, at, :].astype(f32)
            buf[b, at, :] = jnp.where(inside, moved, old).astype(bf16)
            into, sem = ((nk_hbm, k_out), (nv_hbm, v_out))[which]
            stores.append(pltpu.make_async_copy(buf.at[b], into.at[b], sem.at[b]))
            stores[-1].start()
    for copy in stores:
        copy.wait()
    mixed.wait()


def local(
    n, t, tokens, norm_gain, w_query, w_key, w_value, w_output, cache_keys, cache_values,
    map_lambda, out_gain, parents, lengths, accepted,
):
    rows, depth = tokens.shape
    seqs, length, width = cache_keys.shape
    prop = rows // seqs
    both = 2 * prop
    cols = min(n, width // LANES)
    groups = n // cols
    part = rows // groups
    per = seqs // groups
    out_cols = w_output.shape[1]
    inner_n = math.gcd(n, 1 << (n.bit_length() - 1) // 2)
    outer_n = n // inner_n
    stages = outer_n.bit_length() - 1
    vmem = pl.BlockSpec(memory_space=pltpu.VMEM)
    smem = pl.BlockSpec(memory_space=pltpu.SMEM)
    hbm = pl.BlockSpec(memory_space=pl.ANY)
    dma = pltpu.SemaphoreType.DMA
    V = pltpu.VMEM
    grant = 67043328 - 2 * (2 * cache_keys.size + rows * out_cols + n * part * 2 * LANES) - (1 << 14)
    mixed, gathered, keys, values, held, taken = pl.pallas_call(
        functools.partial(main_kernel, n, t, cols, seqs, prop, depth * n, inner_n),
        name="attend",
        out_shape=(
            V((rows, out_cols), bf16),
            V((n // 2, 2, part, 2 * LANES), bf16),
            V(cache_keys.shape, bf16),
            V(cache_values.shape, bf16),
            V(lengths.shape, jnp.int32),
            V(accepted.shape, jnp.int32),
        ),
        in_specs=[hbm] * 13,
        out_specs=(vmem,) * 6,
        scratch_shapes=[
            V(tokens.shape, bf16),
            V((1, depth), f32),
            V((1, map_lambda.shape[0]), f32),
            V((1, width), f32),
            V(parents.shape, jnp.int32),
            pltpu.SMEM(lengths.shape, jnp.int32),
            pltpu.SMEM(accepted.shape, jnp.int32),
            V((3, depth, width), bf16),
            V(w_output.shape, bf16),
            V((per, n, prop, LANES), bf16),
            V((per, n - 1, prop, LANES), bf16),
            V((per, n, prop, LANES), bf16),
            V((inner_n, outer_n, part, 2 * LANES), bf16),
            V((inner_n - 1, outer_n, part, 2 * LANES), bf16),
            V((outer_n, part, 2 * LANES), bf16),
            V((stages, outer_n // 2, part, 2 * LANES), bf16),
            V((n, 1, LANES), f32),
            V((per, n, 2 * prop, LANES), bf16),
            V((per, n - 1, 2 * prop, LANES), bf16),
            V((per, n, 4, LANES), f32),
            V((per, n - 1, 4, LANES), f32),
            V((per, 2 * prop, LANES), f32),
            V((per, 4, LANES), f32),
            V((per, n, prop, LANES), bf16),
            V((per, groups * prop, out_cols), bf16),
            V((per, t - 1, groups * prop, out_cols), bf16),
            dma((9,)),
            dma((4,)),
            dma((seqs,)),
            dma((seqs,)),
            dma, dma,
            dma, dma((per,)),
            dma, dma((per,)),
            dma, dma,
            dma((stages,)), dma((stages,)),
            dma, dma,
            dma, dma,
            dma, dma((per,)),
            dma, dma((per,)),
            dma, dma((per,)),
            dma, dma((per,)),
        ],
        compiler_params=pltpu.CompilerParams(
            collective_id=0, has_side_effects=True, vmem_limit_bytes=grant
        ),
    )(
        tokens, norm_gain[None], map_lambda[None], out_gain[None], parents, lengths, accepted,
        w_query, w_key, w_value, w_output, cache_keys, cache_values,
    )
    mixed, new_keys, new_values, _, _ = pl.pallas_call(
        functools.partial(place_kernel, groups, prop),
        name="place",
        out_shape=(
            jax.ShapeDtypeStruct(mixed.shape, bf16),
            jax.ShapeDtypeStruct(cache_keys.shape, bf16),
            jax.ShapeDtypeStruct(cache_values.shape, bf16),
            V(cache_keys.shape, bf16),
            V(cache_values.shape, bf16),
        ),
        in_specs=[smem, smem, vmem, vmem, vmem, vmem],
        out_specs=(hbm, hbm, hbm, vmem, vmem),
        input_output_aliases={4: 3, 5: 4},
        scratch_shapes=[dma((seqs,))] * 2 + [dma],
        compiler_params=pltpu.CompilerParams(vmem_limit_bytes=16 << 20),
    )(held, taken, mixed, gathered, keys, values)
    return (mixed, new_keys, new_values)


def solution(mesh):
    placed = (
        P(None, "kv"),
        P("kv"),
        P("kv", "tp"),
        P("kv", "tp"),
        P("kv", "tp"),
        P("tp", "kv"),
        P(None, "kv", "tp"),
        P(None, "kv", "tp"),
        P("tp"),
        P("tp"),
        P(),
        P(),
        P(),
    )
    return jax.shard_map(
        functools.partial(local, mesh.shape["kv"], mesh.shape["tp"]),
        mesh=mesh,
        in_specs=placed,
        out_specs=(P(None, "kv"), P(None, "kv", "tp"), P(None, "kv", "tp")),
        check_vma=False,
    )
```

```python
import functools
import math

import jax
import jax.numpy as jnp
from jax import lax
from jax.experimental import pallas as pl
from jax.experimental.pallas import tpu as pltpu
from jax.sharding import PartitionSpec as P

HEAD = 64
QK = 32
LANES = 128
epsilon = 1e-05
masked_low = -1e30
MESH = pl.DeviceIdType.MESH
f32 = jnp.float32
bf16 = jnp.bfloat16


def iota(shape, dim):
    return lax.broadcasted_iota(jnp.int32, shape, dim)


def greet(axes):
    barrier = pltpu.get_barrier_semaphore()
    count = 0
    for axis, n in axes:
        me = lax.axis_index(axis)
        for k in range(1, n):
            pl.semaphore_signal(
                barrier, inc=1, device_id={axis: lax.rem(me + k, n)}, device_id_type=MESH
            )
            count += 1
    return barrier, count


def remote(src, dst, send_sem, recv_sem, axis, to):
    return pltpu.make_async_remote_copy(
        src_ref=src,
        dst_ref=dst,
        send_sem=send_sem,
        recv_sem=recv_sem,
        device_id={axis: to},
        device_id_type=MESH,
    )


def drain(ref, sem):
    pltpu.make_async_copy(ref, ref, sem).wait()


def flip(i, bit):
    return i + bit - 2 * bit * lax.rem(i // bit, 2)


def main_kernel(
    n, t, cols, seqs, prop, features, inner_n,
    tok_hbm, gain_hbm, lam_hbm, out_gain_hbm, parent_hbm, len_hbm, acc_hbm,
    wq_hbm, wk_hbm, wv_hbm, wo_hbm, keys_hbm, vals_hbm,
    out_ref, kv_ref, kbuf, vbuf, len_out, acc_out,
    tok_ref, gain_ref, lam_ref, out_gain_ref, parent_ref, len_ref, acc_ref,
    wbuf, wo_buf, q_part, q_recv, q_all, k_cells, v_cells, kx_recv, vx_recv, kz_recv, vz_recv, v1_recv, sq_all,
    bv, bv_recv, st, st_recv, self_v, self_st, norm_all, out_part, out_recv,
    s_in, w_in, k_in, v_in, sq_s, sq_r, q_s, q_r, qa_s, qa_r, kx_s, kx_r, vx_s, vx_r, kz_s, kz_r, vz_s, vz_r, up_s, up_r, ag_s, ag_r,
    b_s, b_r, st_s, st_r, g_s, g_r, t_s, t_r,
):
    me = lax.axis_index("kv")
    mine = lax.axis_index("tp")
    groups = n // cols
    rows = tok_ref.shape[0]
    part = rows // groups
    per = seqs // groups
    both = 2 * prop
    _, length, width = kbuf.shape
    scale = QK ** (-0.5)
    others = [lax.rem(me + k, n) for k in range(1, n)]
    outer_n = n // inner_n
    half = outer_n // 2
    x, z = lax.rem(me, inner_n), me // inner_n
    toward = 1 - 2 * (z // half)
    peers = []
    for dz in reversed(range(outer_n)):
        for dx in reversed(range(inner_n)):
            if dz or dx:
                to_z = lax.rem(z + toward * dz + outer_n, outer_n)
                peers.append(to_z * inner_n + lax.rem(x + dx, inner_n))
    x_peers = [lax.rem(x + k, inner_n) for k in range(1, inner_n)]
    slot = lax.rem(z, half) * inner_n + x
    flat = half * inner_n - 1
    barrier, count = greet((("kv", n), ("tp", t)))
    weights = [
        pltpu.make_async_copy(src, dst, w_in.at[i])
        for i, (src, dst) in enumerate(
            ((wq_hbm, wbuf.at[0]), (wk_hbm, wbuf.at[1]), (wv_hbm, wbuf.at[2]), (wo_hbm, wo_buf))
        )
    ]
    small = [
        pltpu.make_async_copy(src, dst, s_in.at[i])
        for i, (src, dst) in enumerate(
            (
                (tok_hbm, tok_ref), (gain_hbm, gain_ref), (lam_hbm, lam_ref), (out_gain_hbm, out_gain_ref),
                (parent_hbm, parent_ref), (len_hbm, len_ref), (acc_hbm, acc_ref), (len_hbm, len_out), (acc_hbm, acc_out),
            )
        )
    ]
    order = [r * per + p for p in range(per) for r in range(groups)]
    loads = {}
    for b in order:
        loads[b] = (
            pltpu.make_async_copy(keys_hbm.at[b], kbuf.at[b], k_in.at[b]),
            pltpu.make_async_copy(vals_hbm.at[b], vbuf.at[b], v_in.at[b]),
        )
    for copy in small[:2] + weights[:1] + small[2:] + weights[1:3]:
        copy.start()
    for b in order:
        for copy in loads[b]:
            copy.start()
    weights[3].start()
    for copy in small[:2]:
        copy.wait()

    wide = tok_ref[...].astype(f32)
    square = jnp.sum(wide * wide, axis=1, keepdims=True)
    diagonal = iota((rows, LANES), 0) == iota((rows, LANES), 1)
    as_row = jnp.sum(jnp.where(diagonal, square, 0.0), axis=0, keepdims=True)
    sq_all[me] = as_row
    gained = (wide * gain_ref[...]).astype(bf16)

    def products(which, place):
        weights[which].wait()
        product = jnp.dot(gained, wbuf[which], preferred_element_type=f32)
        for c in range(cols):
            for b in range(seqs):
                place(
                    b % per,
                    c * groups + b // per,
                    product[b * prop : (b + 1) * prop, c * LANES : (c + 1) * LANES].astype(bf16),
                )

    def place_q(p, d, piece):
        q_part[p, d] = piece

    def place_k(p, d, piece):
        k_cells[d % inner_n, d // inner_n, p * prop : (p + 1) * prop] = piece

    def place_v(p, d, piece):
        v_cells[d // inner_n, d % inner_n, p * prop : (p + 1) * prop] = piece

    products(0, place_q)
    pl.semaphore_wait(barrier, count)
    for to in peers:
        remote(sq_all.at[me], sq_all.at[me], sq_s, sq_r, "kv", to).start()
    for p in range(per):
        for to in peers:
            remote(q_part.at[p, to], q_recv.at[p, me], q_s, q_r.at[p], "kv", to).start()
    products(1, place_k)
    for k, to in enumerate(x_peers):
        remote(k_cells.at[to], kx_recv.at[k], kx_s, kx_r, "kv", z * inner_n + to).start()
    products(2, place_v)
    chunks = [z]
    bits = [1 << i for i in range(outer_n.bit_length() - 1)]
    live = {}
    for i in reversed(range(len(bits))):
        live[i] = chunks
        chunks = chunks + [flip(c, bits[i]) for c in chunks]
    near = flip(z, 1) * inner_n + x
    for i, c in enumerate(live[0]):
        remote(v_cells.at[flip(c, 1)], vz_recv.at[i], vz_s.at[0], vz_r.at[0], "kv", near).start()

    lane = iota((1, LANES), 1)
    low = lane < HEAD
    for copy in small[2:]:
        copy.wait()
    own_first = lax.rem(me, groups) * per
    small_eye = iota((prop, prop), 0) == iota((prop, prop), 1)
    parent_rows = []
    for b in range(per):
        line = parent_ref[pl.ds(own_first + b, 1), :]
        parent_rows.append(
            jnp.sum(jnp.where(small_eye, line, 0), axis=1, keepdims=True)
        )
    parent = jnp.concatenate(parent_rows, axis=0)
    shape = (part, part)
    target = jnp.concatenate([p + b * prop for b, p in enumerate(parent_rows)], axis=0)
    link = (parent >= 0) & (target == iota(shape, 1))
    reach = jnp.where(link | (iota(shape, 0) == iota(shape, 1)), 1.0, 0.0)
    power = 1
    while power < prop:
        reach = jnp.minimum(
            jnp.dot(reach.astype(bf16), reach.astype(bf16), preferred_element_type=f32), 1.0
        )
        power *= 2
    lineage = jnp.concatenate([reach] * 4, axis=0) > 0.5

    drain(sq_all.at[pl.ds(0, n - 1)], sq_r)
    squares = sq_all[0]
    for k in range(1, n):
        squares = squares + sq_all[k]
    first = lax.rem(me, groups) * part
    picked = iota((part, LANES), 0) + first == iota((part, LANES), 1)
    mean = jnp.sum(jnp.where(picked, squares, 0.0), axis=1, keepdims=True) / features
    factor = lax.rsqrt(mean + epsilon)
    for p in range(per):
        drain(q_recv.at[p, pl.ds(0, n - 1)], q_r.at[p])
        total = q_part[p, me].astype(f32)
        for d in others:
            total = total + q_recv[p, d].astype(f32)
        q_all[p, me] = (total * factor[p * prop : (p + 1) * prop]).astype(bf16)
        for to in peers:
            remote(q_all.at[p, me], q_all.at[p, me], qa_s, qa_r.at[p], "kv", to).start()

    def add(cells, at, received):
        total = cells[at].astype(f32)
        for piece in received:
            total = total + piece.astype(f32)
        cells[at] = total.astype(bf16)

    def k_after_x():
        drain(kx_recv, kx_r)
        for i in range(outer_n):
            add(k_cells, (x, i), [kx_recv[k, i] for k in range(inner_n - 1)])

    def k_send(s):
        to = flip(z, bits[s]) * inner_n + x
        for i, c in enumerate(live[s]):
            remote(k_cells.at[x, flip(c, bits[s])], kz_recv.at[s, i], kz_s.at[s], kz_r.at[s], "kv", to).start()

    def k_take(s):
        size = len(live[s])
        drain(kz_recv.at[s, pl.ds(0, size)], kz_r.at[s])
        for i, c in enumerate(live[s]):
            add(k_cells, (x, c), [kz_recv[s, i]])

    def v_after_z():
        drain(vz_recv, vz_r.at[0])
        for i, c in enumerate(live[0]):
            for k in range(inner_n):
                add(v_cells, (c, k), [vz_recv[i, k]])
        for k, to in enumerate(x_peers):
            for i, c in enumerate(live[0]):
                remote(v_cells.at[c, to], vx_recv.at[k, i], vx_s, vx_r, "kv", z * inner_n + to).start()

    def v_after_x():
        drain(vx_recv, vx_r)
        for i, c in enumerate(live[0]):
            add(v_cells, (c, x), [vx_recv[k, i] for k in range(inner_n - 1)])

    def v_send(s):
        to = flip(z, bits[s]) * inner_n + x
        for i, c in enumerate(live[s]):
            remote(v_cells.at[flip(c, bits[s]), x], v1_recv.at[s, i], vz_s.at[s], vz_r.at[s], "kv", to).start()

    def v_take(s):
        drain(v1_recv.at[s, pl.ds(0, len(live[s]))], vz_r.at[s])
        for i, c in enumerate(live[s]):
            add(v_cells, (c, x), [v1_recv[s, i]])

    wide_lane = iota((1, 2 * LANES), 1)

    def attend(p):
        stat = jnp.zeros((both, LANES), f32)
        for r in range(groups):
            b = r * per + p
            rel = len_ref[b] + acc_ref[b] - me * length
            visible = iota((1, length), 1) < rel
            for copy in loads[b]:
                copy.wait()
            for g in range(width // (2 * LANES)):
                span = slice(g * 2 * LANES, (g + 1) * 2 * LANES)
                query = jnp.concatenate(
                    [q_all[p, c * groups + r].astype(f32) for c in (2 * g, 2 * g + 1)], axis=1
                )
                spread = jnp.concatenate(
                    [jnp.where(wide_lane // QK == i, query, 0.0) for i in range(2 * LANES // QK)],
                    axis=0,
                ).astype(bf16)
                scores = lax.dot_general(
                    spread, kbuf[b, :, span], (((1,), (1,)), ((), ())), preferred_element_type=f32
                )
                scores = jnp.where(visible, scores * scale, masked_low)
                largest = jnp.max(scores, axis=1, keepdims=True)
                weight = jnp.where(visible, jnp.exp(scores - largest), 0.0)
                total = jnp.sum(weight, axis=1, keepdims=True)
                summed = jnp.dot(weight.astype(bf16), vbuf[b, :, span], preferred_element_type=f32)
                merged = jnp.zeros((both, 2 * LANES), f32)
                for h in range(2 * LANES // HEAD):
                    piece = slice(h * both, (h + 1) * both)
                    merged = jnp.where(wide_lane // HEAD == h, summed[piece], merged)
                    at = ((2 * g + h // 2) * groups + r) * 4 + h % 2
                    stat = jnp.where(lane == at, largest[piece], stat)
                    stat = jnp.where(lane == at + 2, total[piece], stat)
                merged = merged.astype(bf16)
                for c in range(2):
                    bv[p, (2 * g + c) * groups + r] = merged[:, c * LANES : (c + 1) * LANES]
        turned = jnp.transpose(
            jnp.concatenate([stat, jnp.zeros((LANES - both, LANES), f32)], axis=0)
        )
        for d in range(n):
            st[p, d] = turned[4 * d : 4 * d + 4]

    def exchange(p):
        for to in peers:
            remote(st.at[p, to], st_recv.at[p, me], st_s, st_r.at[p], "kv", to).start()
            remote(bv.at[p, to], bv_recv.at[p, me], b_s, b_r.at[p], "kv", to).start()

    def tree():
        key = (k_cells[x, z].astype(f32) * factor).astype(bf16)
        value = (v_cells[z, x].astype(f32) * factor).astype(bf16)
        kv_ref[slot, z // half, :, :LANES] = key
        kv_ref[slot, z // half, :, LANES:] = value
        query = jnp.concatenate([q_all[p, me] for p in range(per)], axis=0).astype(f32)
        spread = jnp.concatenate(
            [jnp.where(lane // QK == i, query, 0.0) for i in range(4)], axis=0
        ).astype(bf16)
        scores = lax.dot_general(
            spread, key, (((1,), (1,)), ((), ())), preferred_element_type=f32
        )
        scores = jnp.where(lineage, scores * scale, masked_low)
        top = jnp.max(scores, axis=1, keepdims=True)
        weight = jnp.where(lineage, jnp.exp(scores - top), 0.0)
        total = jnp.sum(weight, axis=1, keepdims=True)
        summed = jnp.dot(weight.astype(bf16), value, preferred_element_type=f32)
        stat = jnp.zeros((both, LANES), f32)
        for p in range(per):
            cut = [slice(i * part + p * prop, i * part + (p + 1) * prop) for i in range(4)]

            def laid(array, head):
                return jnp.concatenate([array[cut[2 * head]], array[cut[2 * head + 1]]], axis=0)

            self_v[p] = jnp.where(low, laid(summed, 0), laid(summed, 1))
            for h in range(2):
                stat = jnp.where(lane == 4 * p + h, laid(top, h), stat)
                stat = jnp.where(lane == 4 * p + 2 + h, laid(total, h), stat)
        turned = jnp.transpose(
            jnp.concatenate([stat, jnp.zeros((LANES - both, LANES), f32)], axis=0)
        )
        for p in range(per):
            self_st[p] = turned[4 * p : 4 * p + 4]

    def kv_up():
        @pl.when(z < half)
        def _():
            remote(kv_ref.at[slot, 0], kv_ref.at[slot, 0], up_s, up_r, "kv", me + half * inner_n).start()

    def kv_spread():

        @pl.when(z >= half)
        def _():
            drain(kv_ref.at[slot, 0], up_r)
            for k in range(1, flat + 1):
                to = half * inner_n + lax.rem(slot + k, flat + 1)
                remote(kv_ref.at[slot], kv_ref.at[slot], ag_s, ag_r, "kv", to).start()

    def kv_end():

        @pl.when(z < half)
        def _():
            drain(kv_ref.at[slot, 0], up_s)

        @pl.when(z >= half)
        def _():
            for sem in (ag_r, ag_s):
                drain(kv_ref.at[pl.ds(0, flat)], sem)

    col = me // groups
    heads = iota(lam_ref.shape, 1)
    lam_low = jnp.sum(jnp.where(heads == 2 * col, lam_ref[...], 0.0), axis=1, keepdims=True)
    lam_high = jnp.sum(jnp.where(heads == 2 * col + 1, lam_ref[...], 0.0), axis=1, keepdims=True)
    lam = jnp.where(low, lam_low, lam_high)
    gain = out_gain_ref[:, pl.ds(pl.multiple_of(col * LANES, LANES), LANES)]

    def merge(p):
        drain(st_recv.at[p, pl.ds(0, n - 1)], st_r.at[p])
        drain(bv_recv.at[p, pl.ds(0, n - 1)], b_r.at[p])
        stats = [st[p, me]] + [st_recv[p, d] for d in others] + [self_st[p]]
        highest = functools.reduce(jnp.maximum, [a[:2] for a in stats])
        shares = [jnp.exp(a[:2] - highest) for a in stats]
        denominator = functools.reduce(lambda a, b: a + b, [a * b[2:] for a, b in zip(shares, stats)])
        inverse = 1.0 / denominator
        shares = [a * inverse for a in shares]
        filler = jnp.zeros((LANES - 2 * len(shares), LANES), f32)
        turned = jnp.transpose(jnp.concatenate(shares + [filler], axis=0))
        values = [bv[p, me]] + [bv_recv[p, d] for d in others] + [self_v[p]]
        attended = jnp.zeros((both, LANES), f32)
        for i, value in enumerate(values):
            share = jnp.where(low, turned[:both, 2 * i : 2 * i + 1], turned[:both, 2 * i + 1 : 2 * i + 2])
            attended = attended + value.astype(f32) * share
        difference = attended[:prop] - lam * attended[prop:]
        squared = difference * difference
        one = jnp.sum(jnp.where(low, squared, 0.0), axis=1, keepdims=True)
        two = jnp.sum(jnp.where(low, 0.0, squared), axis=1, keepdims=True)
        mean = jnp.where(low, one, two) / HEAD
        norm_all[p, me] = (difference * lax.rsqrt(mean + epsilon) * gain).astype(bf16)
        for to in peers:
            remote(norm_all.at[p, me], norm_all.at[p, me], g_s, g_r.at[p], "kv", to).start()

    def project(p):
        drain(q_recv.at[p, pl.ds(0, n - 1)], g_r.at[p])
        normed = jnp.concatenate(
            [
                jnp.concatenate([norm_all[p, c * groups + r] for r in range(groups)], axis=0)
                for c in range(cols)
            ],
            axis=1,
        )
        out_part[p] = jnp.dot(normed, wo_buf[...], preferred_element_type=f32).astype(bf16)
        for k in range(1, t):
            remote(out_part.at[p], out_recv.at[p, k - 1], t_s, t_r.at[p], "tp", lax.rem(mine + k, t)).start()

    def finish(p):
        drain(out_recv.at[p], t_r.at[p])
        mixed = out_part[p].astype(f32)
        for k in range(t - 1):
            mixed = mixed + out_recv[p, k].astype(f32)
        for r in range(groups):
            b = r * per + p
            out_ref[b * prop : (b + 1) * prop, :] = mixed[r * prop : (r + 1) * prop].astype(bf16)

    k_after_x()
    k_send(0)
    v_after_z()
    last = len(bits) - 1
    steps = [lambda: (v_after_x(), v_send(1))] + [lambda i=i: (k_take(i), k_send(i + 1)) for i in range(last)]
    steps += [lambda i=i: (v_take(i), v_send(i + 1)) for i in range(1, last)]
    for p in range(per):
        drain(q_recv.at[p, pl.ds(0, n - 1)], qa_r.at[p])
        attend(p)
        if p < 2 and steps:
            steps.pop(0)()
        exchange(p)
    for step in steps:
        step()
    k_take(last)
    v_take(last)
    tree()
    kv_up()
    weights[3].wait()
    for p in range(per):
        merge(p)
    kv_spread()
    for p in range(per):
        project(p)
    for p in range(per):
        finish(p)
    kv_end()
    drain(sq_all.at[pl.ds(0, n - 1)], sq_s)
    quiet = q_recv.at[pl.ds(0, per), pl.ds(0, n - 1)]
    for sem in (q_s, qa_s, g_s):
        drain(quiet, sem)
    drain(kx_recv, kx_s)
    drain(vx_recv, vx_s)
    drain(vz_recv, vz_s.at[0])
    for s in range(last + 1):
        drain(kz_recv.at[s, pl.ds(0, len(live[s]))], kz_s.at[s])
        if s:
            drain(v1_recv.at[s, pl.ds(0, len(live[s]))], vz_s.at[s])
    drain(st_recv.at[pl.ds(0, per), pl.ds(0, n - 1)], st_s)
    drain(bv_recv.at[pl.ds(0, per), pl.ds(0, n - 1)], b_s)
    drain(out_recv, t_s)


def place_kernel(
    groups, prop, len_ref, acc_ref, mixed_ref, kv_ref, kbuf_in, vbuf_in, out_hbm, nk_hbm, nv_hbm, kbuf, vbuf,
    k_out, v_out, m_out,
):
    seqs, length, width = kbuf.shape
    cols = width // LANES
    per = seqs // groups
    chunks = kv_ref.shape[0]
    offset = lax.axis_index("kv") * length
    mixed = pltpu.make_async_copy(mixed_ref, out_hbm, m_out)
    mixed.start()
    stores = []
    window = 48
    for b in range(seqs):
        r, begin = b // per, (b % per) * prop
        rel = len_ref[b] + acc_ref[b] - offset
        base = jnp.clip((rel // 16) * 16, 0, length - window)
        at = pl.ds(pl.multiple_of(base, 16), window)
        slot = iota((window, prop), 0) + base - rel
        placing = (slot == iota((window, prop), 1)).astype(bf16)
        slot_col = iota((window, 1), 0) + base - rel
        inside = (slot_col >= 0) & (slot_col < prop)
        for which, buf in enumerate((kbuf, vbuf)):
            fresh = jnp.concatenate(
                [
                    kv_ref[
                        (c * groups + r) % chunks,
                        (c * groups + r) // chunks,
                        begin : begin + prop,
                        which * LANES : (which + 1) * LANES,
                    ]
                    for c in range(cols)
                ],
                axis=1,
            )
            moved = jnp.dot(placing, fresh, preferred_element_type=f32)
            old = buf[b, at, :].astype(f32)
            buf[b, at, :] = jnp.where(inside, moved, old).astype(bf16)
            into, sem = ((nk_hbm, k_out), (nv_hbm, v_out))[which]
            stores.append(pltpu.make_async_copy(buf.at[b], into.at[b], sem.at[b]))
            stores[-1].start()
    for copy in stores:
        copy.wait()
    mixed.wait()


def local(
    n, t, tokens, norm_gain, w_query, w_key, w_value, w_output, cache_keys, cache_values,
    map_lambda, out_gain, parents, lengths, accepted,
):
    rows, depth = tokens.shape
    seqs, length, width = cache_keys.shape
    prop = rows // seqs
    both = 2 * prop
    cols = min(n, width // LANES)
    groups = n // cols
    part = rows // groups
    per = seqs // groups
    out_cols = w_output.shape[1]
    inner_n = math.gcd(n, 1 << (n.bit_length() - 1) // 2)
    outer_n = n // inner_n
    stages = outer_n.bit_length() - 1
    vmem = pl.BlockSpec(memory_space=pltpu.VMEM)
    smem = pl.BlockSpec(memory_space=pltpu.SMEM)
    hbm = pl.BlockSpec(memory_space=pl.ANY)
    dma = pltpu.SemaphoreType.DMA
    V = pltpu.VMEM
    grant = 67043328 - 2 * (2 * cache_keys.size + rows * out_cols + n * part * 2 * LANES) - (1 << 14)
    mixed, gathered, keys, values, held, taken = pl.pallas_call(
        functools.partial(main_kernel, n, t, cols, seqs, prop, depth * n, inner_n),
        name="attend",
        out_shape=(
            V((rows, out_cols), bf16),
            V((n // 2, 2, part, 2 * LANES), bf16),
            V(cache_keys.shape, bf16),
            V(cache_values.shape, bf16),
            V(lengths.shape, jnp.int32),
            V(accepted.shape, jnp.int32),
        ),
        in_specs=[hbm] * 13,
        out_specs=(vmem,) * 6,
        scratch_shapes=[
            V(tokens.shape, bf16),
            V((1, depth), f32),
            V((1, map_lambda.shape[0]), f32),
            V((1, width), f32),
            V(parents.shape, jnp.int32),
            pltpu.SMEM(lengths.shape, jnp.int32),
            pltpu.SMEM(accepted.shape, jnp.int32),
            V((3, depth, width), bf16),
            V(w_output.shape, bf16),
            V((per, n, prop, LANES), bf16),
            V((per, n, prop, LANES), bf16),
            V((per, n, prop, LANES), bf16),
            V((inner_n, outer_n, part, LANES), bf16),
            V((outer_n, inner_n, part, LANES), bf16),
            V((inner_n - 1, outer_n, part, LANES), bf16),
            V((inner_n - 1, outer_n // 2, part, LANES), bf16),
            V((stages, outer_n // 2, part, LANES), bf16),
            V((outer_n // 2, inner_n, part, LANES), bf16),
            V((stages, outer_n // 2, part, LANES), bf16),
            V((n, 1, LANES), f32),
            V((per, n, 2 * prop, LANES), bf16),
            V((per, n, 2 * prop, LANES), bf16),
            V((per, n, 4, LANES), f32),
            V((per, n, 4, LANES), f32),
            V((per, 2 * prop, LANES), f32),
            V((per, 4, LANES), f32),
            V((per, n, prop, LANES), bf16),
            V((per, groups * prop, out_cols), bf16),
            V((per, t - 1, groups * prop, out_cols), bf16),
            dma((9,)),
            dma((4,)),
            dma((seqs,)),
            dma((seqs,)),
            dma, dma,
            dma, dma((per,)),
            dma, dma((per,)),
            dma, dma,
            dma, dma,
            dma((stages,)), dma((stages,)),
            dma((stages,)), dma((stages,)),
            dma, dma,
            dma, dma,
            dma, dma((per,)),
            dma, dma((per,)),
            dma, dma((per,)),
            dma, dma((per,)),
        ],
        compiler_params=pltpu.CompilerParams(
            collective_id=0, has_side_effects=True, vmem_limit_bytes=grant
        ),
    )(
        tokens, norm_gain[None], map_lambda[None], out_gain[None], parents, lengths, accepted,
        w_query, w_key, w_value, w_output, cache_keys, cache_values,
    )
    mixed, new_keys, new_values, _, _ = pl.pallas_call(
        functools.partial(place_kernel, groups, prop),
        name="place",
        out_shape=(
            jax.ShapeDtypeStruct(mixed.shape, bf16),
            jax.ShapeDtypeStruct(cache_keys.shape, bf16),
            jax.ShapeDtypeStruct(cache_values.shape, bf16),
            V(cache_keys.shape, bf16),
            V(cache_values.shape, bf16),
        ),
        in_specs=[smem, smem, vmem, vmem, vmem, vmem],
        out_specs=(hbm, hbm, hbm, vmem, vmem),
        input_output_aliases={4: 3, 5: 4},
        scratch_shapes=[dma((seqs,))] * 2 + [dma],
        compiler_params=pltpu.CompilerParams(vmem_limit_bytes=16 << 20),
    )(held, taken, mixed, gathered, keys, values)
    return (mixed, new_keys, new_values)


def solution(mesh):
    placed = (
        P(None, "kv"),
        P("kv"),
        P("kv", "tp"),
        P("kv", "tp"),
        P("kv", "tp"),
        P("tp", "kv"),
        P(None, "kv", "tp"),
        P(None, "kv", "tp"),
        P("tp"),
        P("tp"),
        P(),
        P(),
        P(),
    )
    return jax.shard_map(
        functools.partial(local, mesh.shape["kv"], mesh.shape["tp"]),
        mesh=mesh,
        in_specs=placed,
        out_specs=(P(None, "kv"), P(None, "kv", "tp"), P(None, "kv", "tp")),
        check_vma=False,
    )
```
